512 devices in a mesh: sp: 128 (over z, x, core), tp: 4 (over y).
Axes of the slice: x: 4, y: 4, z: 16, core: 2. Of those that a mesh axis runs over, the one named last changes fastest.
Arguments:
- tokens: bfloat16 [32768, 2048], P('sp', 'tp'), may hold values from -6 to 6
- segments: int32 [32768], P('sp'), may hold values from 0 to 63, never falling along the last dimension, each value on 1 to 1024 neighbouring positions
- in_gain: float32 [2, 2048], replicated, may hold values from 0.1 to 1.9
- w_value: bfloat16 [2, 2048, 1024], P(None, 'sp', 'tp'), may hold values from -0.125 to 0.125
- w_gate: bfloat16 [2, 2048, 1024], P(None, 'sp', 'tp'), may hold values from -0.125 to 0.125
- conv_taps: float32 [2, 129, 1024], P(None, None, 'tp'), may hold values from -4 to 4, as said below
- norm_gain: float32 [2, 1024], P(None, 'tp'), may hold values from 0.1 to 1.9
- w_out: bfloat16 [2, 1024, 2048], P(None, 'tp', 'sp'), may hold values from -0.1875 to 0.1875
Outputs:
- mixed: bfloat16 [32768, 2048], P('sp', 'tp')
The draws below stay inside these ranges and needn't reach their ends.
Inputs may be any that keep to these rules, and one draw needn't show every extreme that they name: `segments`: document numbers never fall along the sequence; each document has 1 to 1024 positions, one has exactly 1024. `conv_taps`: real-valued taps.
All inputs are finite; a program needn't handle non-finite values.
Results may differ from the reference program's by a relative error of at most 0.014.
Values may be sent and summed in bfloat16 or wider, within the bound.
No kernel may reach another device: no remote copies, remote signals or barrier semaphores. Data moves between devices by JAX's collectives and lax.ppermute only.
A program may use at most 64 MiB of HBM per device.

```python
import math
import jax
import jax.numpy as jnp
import numpy as np
from jax import lax

D = 2048
CF = 1024
KW = 129
LAYERS = 2
TOKENS = 32768
CF_DEV = 256
DOCS = 64
DOC_MOST = 1024
N_TP = 4


def draw_conv_taps(key, part):
    first, second = jax.random.split(key, 2)
    group_scale = jnp.exp(jax.random.uniform(first, (8,), jnp.float32, jnp.log(0.3), jnp.log(3.0)))
    channel_scale = jnp.repeat(group_scale, CF // 8)
    base = jnp.clip(jax.random.normal(second, (LAYERS, KW, CF), jnp.float32), -4.0, 4.0)
    return (base * channel_scale * KW ** (-0.5)).astype(jnp.float32)


def block_scale(stream_key, extent, cuts, low, high):
    level, own = 1.0, jax.random.fold_in(stream_key, 6)
    for dim, parts in cuts:
        heights = jnp.exp(jax.random.uniform(jax.random.fold_in(own, dim), (parts,), jnp.float32, low / len(cuts), high / len(cuts)))
        level = level * jnp.repeat(heights, extent[dim] // parts).reshape([-1 if axis == dim else 1 for axis in range(len(extent))])
    return level


def length_profile(number_of, total, bound, lean):
    weights = [(1 << 20) // math.isqrt(grade ** lean) + 1 for grade in range(2, number_of + 1)]
    rest, given = total - bound - (number_of - 1), [1] * (number_of - 1)
    while rest > 0:
        candidates = [i for i in range(number_of - 1) if given[i] < bound]
        whole, remaining = sum([weights[i] for i in candidates]), rest
        for i in candidates:
            more = min(bound - given[i], max(1, remaining * weights[i] // whole), rest)
            given[i] = given[i] + more
            rest = rest - more
    return np.array([bound] + given)


def ragged(own_key, number_of, total, most, slope):
    if number_of == 2:
        one = jax.random.randint(own_key, (), max(1, total - most), min(most, total - 1) + 1)
        return jnp.stack([one, total - one])
    lengths = jnp.asarray(length_profile(number_of, total, most, slope), jnp.int32)
    couples = (number_of - 1) // 2
    giver, taker = lengths[1:1 + 2 * couples:2], lengths[2:2 + 2 * couples:2]
    margin = jnp.minimum(giver - 1, most - taker)
    moved = jax.random.randint(jax.random.fold_in(own_key, 1), (couples,), 0, 1 << 20) % (margin + 1)
    lengths = lengths.at[1:1 + 2 * couples:2].set(giver - moved).at[2:2 + 2 * couples:2].set(taker + moved)
    return lengths[jax.random.permutation(jax.random.fold_in(own_key, 2), number_of)]


def bell_draw(rng, extent, spread, reach, shards=(), dtype=jnp.bfloat16):
    drawn = spread * jax.random.normal(rng, extent, jnp.float32)
    if shards:
        drawn = drawn * block_scale(rng, extent, shards, -0.22, 0.18)
    return jnp.clip(drawn, -reach, reach).astype(dtype)


def setup_inputs(seed: int = 0) -> dict:
    arg_keys = jax.random.split(jax.random.key(seed), 9)
    tokens = bell_draw(arg_keys[0], (TOKENS, D), 1.0, 6.0, ((0, 128), (1, 4)))
    segments = jnp.searchsorted(jnp.cumsum(ragged(arg_keys[1], DOCS, TOKENS, DOC_MOST, 2)), jnp.arange(TOKENS), side="right").astype(jnp.int32)
    in_gain = jnp.clip(1.0 + 0.18 * jax.random.normal(arg_keys[2], (LAYERS, D), jnp.float32), 0.1, 1.9)
    w_value = bell_draw(arg_keys[3], (LAYERS, D, CF), D ** -0.5, 0.125, ((1, 128), (2, 4)))
    w_gate = bell_draw(arg_keys[4], (LAYERS, D, CF), D ** -0.5, 0.125, ((1, 128), (2, 4)))
    conv_taps = draw_conv_taps(jax.random.fold_in(arg_keys[8], 71), 0)
    norm_gain = jnp.clip(1.0 + 0.18 * jax.random.normal(arg_keys[6], (LAYERS, CF), jnp.float32), 0.1, 1.9)
    w_out = bell_draw(arg_keys[7], (LAYERS, CF, D), CF ** -0.5, 0.1875, ((1, 4), (2, 128)))
    return {"tokens": tokens, "segments": segments, "in_gain": in_gain, "w_value": w_value, "w_gate": w_gate, "conv_taps": conv_taps, "norm_gain": norm_gain, "w_out": w_out}


EPSILON = 0.01

def rms_rows(stream, gain):
    wide_vals = stream.astype(jnp.float32)
    scale = lax.rsqrt(lax.optimization_barrier(jnp.mean(wide_vals * wide_vals, axis=-1, keepdims=True)) + EPSILON)
    return (wide_vals * scale * gain).astype(jnp.bfloat16)

def reference(tokens, segments, in_gain, w_value, w_gate, conv_taps, norm_gain, w_out):
    fringe = (KW - 1) // 2
    seg_pad = jnp.pad(segments, (fringe, fringe), constant_values=-1)
    stream = tokens
    for layer_idx in range(LAYERS):
        normed = rms_rows(stream, in_gain[layer_idx])
        value_pre = jnp.dot(normed, w_value[layer_idx], preferred_element_type=jnp.float32)
        gate_pre = jnp.dot(normed, w_gate[layer_idx], preferred_element_type=jnp.float32)
        gated = (value_pre * jax.nn.sigmoid(gate_pre)).astype(jnp.bfloat16)
        padded = jnp.pad(gated.astype(jnp.float32), ((fringe, fringe), (0, 0)))
        tap_table = conv_taps[layer_idx]

        def add_tap(shift_idx, running):
            shift_idx = jnp.asarray(shift_idx).astype(jnp.int32)
            window = lax.dynamic_slice_in_dim(padded, shift_idx, TOKENS, 0)
            same_doc = lax.dynamic_slice_in_dim(seg_pad, shift_idx, TOKENS, 0) == segments
            tap_row = lax.dynamic_slice_in_dim(tap_table, shift_idx, 1, 0)
            return running + jnp.where(same_doc[:, None], window * tap_row, jnp.float32(0.0))
        conv = lax.fori_loop(0, KW, add_tap, jnp.zeros((TOKENS, CF), jnp.float32))
        row_mean = lax.optimization_barrier(jnp.mean(conv, axis=-1, keepdims=True))
        centred = conv - row_mean
        row_var = lax.optimization_barrier(jnp.mean(centred * centred, axis=-1, keepdims=True))
        activated = jax.nn.silu(centred * lax.rsqrt(row_var + EPSILON) * norm_gain[layer_idx]).astype(jnp.bfloat16)
        out_weight = w_out[layer_idx]

        def add_block(block_idx, running):
            first = (jnp.asarray(block_idx) * CF_DEV).astype(jnp.int32)
            columns = lax.dynamic_slice_in_dim(activated, first, CF_DEV, 1)
            weight_rows = lax.dynamic_slice_in_dim(out_weight, first, CF_DEV, 0)
            partial_value = jnp.dot(columns, weight_rows, preferred_element_type=jnp.float32)
            return running + lax.optimization_barrier(partial_value.astype(jnp.bfloat16)).astype(jnp.float32)
        summed = lax.fori_loop(0, N_TP, add_block, jnp.zeros((TOKENS, D), jnp.float32))
        stream = (stream.astype(jnp.float32) + summed).astype(jnp.bfloat16)
    return stream
```

```python
import functools

import jax
import jax.numpy as jnp
from jax import lax
from jax.experimental import pallas as pl
from jax.experimental.pallas import tpu as pltpu
from jax.sharding import Mesh
from jax.sharding import PartitionSpec as P

D = 2048
CF = 1024
KW = 129
LAYERS = 2
EPSILON = 0.01
R = (KW - 1) // 2
SP = ("z", "x", "c")
NZ, NX, NC, NT = 16, 4, 2, 4
TOK = 256
CH = 256
FD = 512
LANES = 128
TILE = 64

F32 = jnp.float32
BF16 = jnp.bfloat16
LIMIT = pltpu.CompilerParams(vmem_limit_bytes=24 * 1024 * 1024)
VMEM = pl.BlockSpec(memory_space=pltpu.VMEM)
SMEM = pl.BlockSpec(memory_space=pltpu.SMEM)


def assemble(own_ref, other_ref, core, scratch):
    for x in range(NX):
        scratch[:, x, core] = own_ref[x]
        scratch[:, x, 1 - core] = other_ref[x]


def gate_kernel(core_ref, g_ref, gain_ref, own_ref, other_ref, out_ref, w_ref):
    assemble(own_ref, other_ref, core_ref[0], w_ref)
    wide = [g_ref[y].astype(F32) for y in range(NT)]
    square = sum(jnp.sum(v * v, axis=1, keepdims=True) for v in wide)
    scale = lax.rsqrt(square * (1.0 / D) + EPSILON)
    pre = jnp.zeros((TOK, 2 * CH), F32)
    step = NZ // NT
    for y in range(NT):
        normed = (wide[y] * scale * gain_ref[y : y + 1, :]).astype(BF16)
        w = w_ref[y * step : (y + 1) * step].reshape(FD, 2 * CH)
        pre = pre + jnp.dot(normed, w, preferred_element_type=F32)
    out_ref[...] = (pre[:, :CH] * jax.nn.sigmoid(pre[:, CH:])).astype(BF16)


def gate(core, gathered, gain, own, other):
    return pl.pallas_call(
        gate_kernel,
        out_shape=jax.ShapeDtypeStruct((TOK, CH), BF16),
        in_specs=[SMEM, VMEM, VMEM, VMEM, VMEM],
        out_specs=VMEM,
        scratch_shapes=[pltpu.VMEM((NZ, NX, NC, 16, 2 * CH), BF16)],
        name="gate",
        compiler_params=LIMIT,
    )(core, gathered, gain, own, other)


def conv_kernel(before_ref, mid_ref, after_ref, seg_ref, taps_ref, conv_ref, stat_ref, x_ref):
    for h in range(CH // LANES):
        cols = slice(h * LANES, (h + 1) * LANES)
        x_ref[h, 0:R] = before_ref[:, cols].astype(F32)
        x_ref[h, R : R + TOK] = mid_ref[:, cols].astype(F32)
        x_ref[h, R + TOK : R + TOK + R] = after_ref[:, cols].astype(F32)

    def tile(i, carry):
        first = pl.multiple_of(i * TILE, TILE)
        own = seg_ref[pl.ds(first + R, TILE), :]
        acc = [jnp.zeros((TILE, LANES), F32) for _ in range(CH // LANES)]
        for k in range(KW):
            same = seg_ref[pl.ds(first + k, TILE), :] == own
            for h in range(CH // LANES):
                tap = taps_ref[k : k + 1, h * LANES : (h + 1) * LANES]
                window = x_ref[h, pl.ds(first + k, TILE), :]
                acc[h] = acc[h] + jnp.where(same, window * tap, 0.0)
        for h in range(CH // LANES):
            conv_ref[pl.ds(first, TILE), h * LANES : (h + 1) * LANES] = acc[h]
        return carry

    lax.fori_loop(0, TOK // TILE, tile, 0)
    conv = conv_ref[...]
    ones = jnp.ones((8, CH), F32)
    dims = (((1,), (1,)), ((), ()))
    total = lax.dot_general(ones, conv, dims, precision=lax.Precision.HIGHEST, preferred_element_type=F32)
    square = lax.dot_general(ones, conv * conv, dims, precision=lax.Precision.HIGHEST, preferred_element_type=F32)
    stat_ref[0:1, :] = total[0:1, :]
    stat_ref[1:2, :] = square[0:1, :]


def convolve(before, mid, after, seg, taps):
    return pl.pallas_call(
        conv_kernel,
        out_shape=(jax.ShapeDtypeStruct((TOK, CH), F32), jax.ShapeDtypeStruct((2, TOK), F32)),
        in_specs=[VMEM] * 5,
        out_specs=(VMEM, VMEM),
        scratch_shapes=[pltpu.VMEM((CH // LANES, TOK + 2 * R, LANES), F32)],
        name="conv",
        compiler_params=LIMIT,
    )(before, mid, after, seg, taps)


def out_kernel(core_ref, conv_ref, stat_ref, gain_ref, own_ref, other_ref, out_ref, w_ref):
    assemble(own_ref, other_ref, core_ref[0], w_ref)
    stat = stat_ref[...]
    kind = lax.broadcasted_iota(jnp.int32, (2 * NT, CH), 0) % 2
    dims = (((0,), (0,)), ((), ()))

    def spread(which):
        pick = jnp.where(kind == which, 1.0, 0.0).astype(F32)
        return lax.dot_general(stat, pick, dims, precision=lax.Precision.HIGHEST, preferred_element_type=F32)

    mean = spread(0) * (1.0 / CF)
    var = jnp.maximum(spread(1) * (1.0 / CF) - mean * mean, 0.0)
    v = (conv_ref[...] - mean) * lax.rsqrt(var + EPSILON) * gain_ref[...]
    act = jax.nn.silu(v).astype(BF16)
    step = NZ // NT
    for y in range(NT):
        w = w_ref[y * step : (y + 1) * step].reshape(FD, CH)
        part = lax.dot_general(act, w, (((1,), (1,)), ((), ())), preferred_element_type=F32)
        out_ref[y] = part.astype(BF16)


def project(core, conv, stat, gain, own, other):
    return pl.pallas_call(
        out_kernel,
        out_shape=jax.ShapeDtypeStruct((NT, TOK, FD), BF16),
        in_specs=[SMEM, VMEM, VMEM, VMEM, VMEM, VMEM],
        out_specs=VMEM,
        scratch_shapes=[pltpu.VMEM((NZ, NX, NC, 16, CH), BF16)],
        name="project",
        compiler_params=LIMIT,
    )(core, conv, stat, gain, own, other)


def add_kernel(copies, stream_ref, parts_ref, out_ref):
    total = stream_ref[...].astype(F32) + sum(parts_ref[y].astype(F32) for y in range(NT))
    total = total.astype(BF16)
    if copies == 1:
        out_ref[...] = total
    else:
        for y in range(copies):
            out_ref[y] = total


def add_parts(stream, parts, copies):
    shape = (TOK, FD) if copies == 1 else (copies, TOK, FD)
    return pl.pallas_call(
        functools.partial(add_kernel, copies),
        out_shape=jax.ShapeDtypeStruct(shape, BF16),
        in_specs=[VMEM, VMEM],
        out_specs=VMEM,
        name="add_parts",
        compiler_params=LIMIT,
    )(stream, parts)


def copies_of(x, n):
    return jnp.broadcast_to(x[None], (n, *x.shape))


def swap_core(x):
    return lax.ppermute(x, "c", [(0, 1), (1, 0)])


def exchange(x, axis):
    return lax.all_to_all(x, axis, 0, 0, tiled=True)


def shift_ring(x, step):
    return lax.ppermute(x, "x", [(i, (i + step) % NX) for i in range(NX)])


def neighbours(x):
    n = NZ * NX * NC
    up = [(i, i + 1) for i in range(n - 1)]
    down = [(j, i) for i, j in up]
    before = lax.ppermute(x[x.shape[0] - R :], SP, up)
    after = lax.ppermute(x[:R], SP, down)
    return before, after


def after_(x, *others):
    return lax.optimization_barrier((x, *others))[0]


def per_device(tokens, segments, in_gain, w_value, w_gate, conv_taps, norm_gain, w_out):
    core = lax.axis_index("c").astype(jnp.int32).reshape(1)
    gains = in_gain.reshape(LAYERS, NT, FD)

    out_t = jnp.swapaxes(w_out, 1, 2)
    own = jnp.concatenate(
        [w_value[0], w_gate[0], out_t[0], w_value[1], w_gate[1], out_t[1]], axis=1
    )
    gathered = exchange(copies_of(tokens, NT), "tp")
    column = lax.all_gather(own, "z", axis=0, tiled=True)

    def over_x(piece):
        width = piece.shape[1]
        return exchange(copies_of(piece, NX), "x").reshape(NX, NZ, 16, width)

    vg0 = over_x(column[:, : 2 * CH])
    vg0_other = swap_core(vg0)
    out0 = over_x(after_(column[:, 2 * CH : 3 * CH], vg0))
    seg_before, seg_after = neighbours(after_(segments, column))
    seg_wide = jnp.concatenate([seg_before, segments, seg_after])
    seg_lanes = jnp.broadcast_to(seg_wide[:, None], (TOK + 2 * R, LANES))

    stream = tokens
    rest = None
    for layer in range(LAYERS):
        if layer == 0:
            vg, vg_other = vg0, vg0_other
        else:
            vg, vg_other = vg1, vg1_other
        gated = gate(core, gathered, gains[layer], vg, vg_other)
        before, after = neighbours(gated)
        conv, stat = convolve(before, gated, after, seg_lanes, conv_taps[layer])
        if layer == 0:
            out, out_other = out0, swap_core(out0)
        else:
            out, out_other = out1, out1_other
        stats = lax.all_gather(stat, "tp", axis=0, tiled=True)
        parts = project(core, conv, stats, norm_gain[layer].reshape(1, CH), out, out_other)
        received = exchange(parts, "tp")
        if layer == 0:
            rest = over_x(after_(column[:, 3 * CH :], out0))
            rest_other = swap_core(rest)
            vg1, out1 = rest[..., : 2 * CH], rest[..., 2 * CH :]
            vg1_other, out1_other = rest_other[..., : 2 * CH], rest_other[..., 2 * CH :]
            spread = add_parts(stream, received, NT)
            stream = spread[0]
            gathered = exchange(spread, "tp")
        else:
            stream = add_parts(stream, received, 1)
    return stream


def solution(mesh):
    fine = Mesh(mesh.devices.reshape(NZ, NX, NC, NT), ("z", "x", "c", "tp"))
    in_specs = (
        P(SP, "tp"),
        P(SP),
        P(),
        P(None, SP, "tp"),
        P(None, SP, "tp"),
        P(None, None, "tp"),
        P(None, "tp"),
        P(None, "tp", SP),
    )
    out_specs = P(SP, "tp")
    return jax.shard_map(
        per_device, mesh=fine, in_specs=in_specs, out_specs=out_specs, check_vma=False
    )
```

```python
import functools

import jax
import jax.numpy as jnp
from jax import lax
from jax.experimental import pallas as pl
from jax.experimental.pallas import tpu as pltpu
from jax.sharding import Mesh
from jax.sharding import PartitionSpec as P


D = 2048
CF = 1024
KW = 129
LAYERS = 2
EPSILON = 0.01
R = (KW - 1) // 2
SP = ("z", "x", "c")
NZ, NX, NC, NT = 16, 4, 2, 4
TOK = 256
CH = 256
FD = 512
LANES = 128
TILE = 64
STEPS = (0, 1, 3, 2)

F32 = jnp.float32
BF16 = jnp.bfloat16
LIMIT = pltpu.CompilerParams(vmem_limit_bytes=16 * 1024 * 1024)
VMEM = pl.BlockSpec(memory_space=pltpu.VMEM)
SMEM = pl.BlockSpec(memory_space=pltpu.SMEM)


def assemble(rotated, at_ref, own_ref, other_ref, cols, scratch):
    core = at_ref[0]
    width = cols.stop - cols.start
    for i in range(NX):
        x = lax.rem(at_ref[2] + (NX - STEPS[i]), NX) if rotated else i
        scratch[:, x, core] = own_ref[i, :, cols].reshape(NZ, 16, width)
        scratch[:, x, 1 - core] = other_ref[i, :, cols].reshape(NZ, 16, width)


def pack_kernel(value_ref, gate_ref, out_ref, packed_ref):
    at = 0
    for layer in range(LAYERS):
        for ref in (value_ref, gate_ref, out_ref):
            packed_ref[:, at : at + CH] = ref[layer]
            at += CH


def pack(value, gate_, out):
    return pl.pallas_call(
        pack_kernel,
        out_shape=jax.ShapeDtypeStruct((16, 6 * CH), BF16),
        in_specs=[VMEM] * 3,
        out_specs=VMEM,
        name="pack",
        compiler_params=LIMIT,
    )(value, gate_, out)


def gate_kernel(layer, at_ref, p0_ref, p1_ref, p2_ref, p3_ref, gain_ref, own_ref, other_ref, out_ref, w_ref):
    assemble(layer > 0, at_ref, own_ref, other_ref, slice(0, 2 * CH), w_ref)
    wide = [ref[...].astype(F32) for ref in (p0_ref, p1_ref, p2_ref, p3_ref)]
    square = sum(jnp.sum(v * v, axis=1, keepdims=True) for v in wide)
    scale = lax.rsqrt(square * (1.0 / D) + EPSILON)
    pre = jnp.zeros((TOK, 2 * CH), F32)
    part = NZ // NT
    for v, step in zip(wide, STEPS):
        y = lax.rem(at_ref[1] + (NT - step), NT)
        gain = gain_ref[layer : layer + 1, pl.ds(pl.multiple_of(y * FD, FD), FD)]
        normed = (v * scale * gain).astype(BF16)
        w = w_ref[pl.ds(y * part, part)].reshape(FD, 2 * CH)
        pre = pre + jnp.dot(normed, w, preferred_element_type=F32)
    out_ref[...] = (pre[:, :CH] * jax.nn.sigmoid(pre[:, CH:])).astype(BF16)


def gate(layer, at, pieces, gain, own, other):
    return pl.pallas_call(
        functools.partial(gate_kernel, layer),
        out_shape=jax.ShapeDtypeStruct((TOK, CH), BF16),
        in_specs=[SMEM] + [VMEM] * 7,
        out_specs=VMEM,
        scratch_shapes=[pltpu.VMEM((NZ, NX, NC, 16, 2 * CH), BF16)],
        name="gate",
        compiler_params=LIMIT,
    )(at, *pieces, gain, own, other)


def conv_kernel(layer, before_ref, mid_ref, after_ref, seg_ref, taps_ref, conv_ref, stat_ref, x_ref):
    for h in range(CH // LANES):
        cols = slice(h * LANES, (h + 1) * LANES)
        x_ref[h, 0:R] = before_ref[:, cols].astype(F32)
        x_ref[h, R : R + TOK] = mid_ref[:, cols].astype(F32)
        x_ref[h, R + TOK : R + TOK + R] = after_ref[:, cols].astype(F32)

    def tile(i, carry):
        first = pl.multiple_of(i * TILE, TILE)
        own = seg_ref[pl.ds(first + R, TILE), :]
        acc = [jnp.zeros((TILE, LANES), F32) for _ in range(CH // LANES)]
        for k in range(KW):
            same = seg_ref[pl.ds(first + k, TILE), :] == own
            for h in range(CH // LANES):
                tap = taps_ref[k, layer : layer + 1, h * LANES : (h + 1) * LANES]
                window = x_ref[h, pl.ds(first + k, TILE), :]
                acc[h] = acc[h] + jnp.where(same, window * tap, 0.0)
        for h in range(CH // LANES):
            conv_ref[pl.ds(first, TILE), h * LANES : (h + 1) * LANES] = acc[h]
        return carry

    lax.fori_loop(0, TOK // TILE, tile, 0)
    conv = conv_ref[...]
    ones = jnp.ones((8, CH), F32)
    dims = (((1,), (1,)), ((), ()))
    total = lax.dot_general(ones, conv, dims, precision=lax.Precision.HIGHEST, preferred_element_type=F32)
    square = lax.dot_general(ones, conv * conv, dims, precision=lax.Precision.HIGHEST, preferred_element_type=F32)
    stat_ref[0:1, :] = total[0:1, :]
    stat_ref[1:2, :] = square[0:1, :]


def convolve(layer, before, mid, after, seg, taps):
    return pl.pallas_call(
        functools.partial(conv_kernel, layer),
        out_shape=(jax.ShapeDtypeStruct((TOK, CH), F32), jax.ShapeDtypeStruct((2, TOK), F32)),
        in_specs=[VMEM] * 5,
        out_specs=(VMEM, VMEM),
        scratch_shapes=[pltpu.VMEM((CH // LANES, TOK + 2 * R, LANES), F32)],
        name="conv",
        compiler_params=LIMIT,
    )(before, mid, after, seg, taps)


def out_kernel(layer, at_ref, conv_ref, stat_ref, gain_ref, own_ref, other_ref, out_ref, w_ref):
    assemble(layer > 0, at_ref, own_ref, other_ref, slice(2 * CH, 3 * CH), w_ref)
    stat = stat_ref[...]
    kind = lax.broadcasted_iota(jnp.int32, (2 * NT, CH), 0) % 2
    dims = (((0,), (0,)), ((), ()))

    def spread(which):
        pick = jnp.where(kind == which, 1.0, 0.0).astype(F32)
        return lax.dot_general(stat, pick, dims, precision=lax.Precision.HIGHEST, preferred_element_type=F32)

    mean = spread(0) * (1.0 / CF)
    var = jnp.maximum(spread(1) * (1.0 / CF) - mean * mean, 0.0)
    v = (conv_ref[...] - mean) * lax.rsqrt(var + EPSILON) * gain_ref[layer : layer + 1, :]
    act = jax.nn.silu(v).astype(BF16)
    step = NZ // NT
    for y in range(NT):
        w = w_ref[y * step : (y + 1) * step].reshape(FD, CH)
        part = lax.dot_general(act, w, (((1,), (1,)), ((), ())), preferred_element_type=F32)
        out_ref[y] = part.astype(BF16)


def project(layer, at, conv, stat, gain, own, other):
    return pl.pallas_call(
        functools.partial(out_kernel, layer),
        out_shape=jax.ShapeDtypeStruct((NT, TOK, FD), BF16),
        in_specs=[SMEM, VMEM, VMEM, VMEM, VMEM, VMEM],
        out_specs=VMEM,
        scratch_shapes=[pltpu.VMEM((NZ, NX, NC, 16, CH), BF16)],
        name="project",
        compiler_params=LIMIT,
    )(at, conv, stat, gain, own, other)


def add_kernel(stream_ref, parts_ref, out_ref):
    total = stream_ref[...].astype(F32) + sum(parts_ref[y].astype(F32) for y in range(NT))
    out_ref[...] = total.astype(BF16)


def add_parts(stream, parts):
    return pl.pallas_call(
        add_kernel,
        out_shape=jax.ShapeDtypeStruct((TOK, FD), BF16),
        in_specs=[VMEM, VMEM],
        out_specs=VMEM,
        name="add_parts",
        compiler_params=LIMIT,
    )(stream, parts)


def copies_of(x, n):
    return jnp.broadcast_to(x[None], (n, *x.shape))


def swap_core(x):
    return lax.ppermute(x, "c", [(0, 1), (1, 0)])


def exchange(x, axis):
    return lax.all_to_all(x, axis, 0, 0, tiled=True)


def ring(x, axis):
    n = lax.axis_size(axis)
    pieces = [x]
    for step in STEPS[1:]:
        pieces.append(lax.ppermute(x, axis, [(i, (i + step) % n) for i in range(n)]))
    return pieces


def neighbours(x):
    n = NZ * NX * NC
    up = [(i, i + 1) for i in range(n - 1)]
    down = [(j, i) for i, j in up]
    before = lax.ppermute(x[x.shape[0] - R :], SP, up)
    after = lax.ppermute(x[:R], SP, down)
    return before, after


def after_(x, *others):
    return lax.optimization_barrier((x, *others))[0]


def program(tokens, segments, in_gain, w_value, w_gate, conv_taps, norm_gain, w_out):
    at = jnp.stack([lax.axis_index(a).astype(jnp.int32) for a in ("c", "tp", "x")])

    out_t = jnp.swapaxes(w_out, 1, 2)
    own = pack(w_value, w_gate, out_t)
    column = lax.all_gather(own, "z", axis=0, tiled=True)
    first = exchange(copies_of(column[:, : 3 * CH], NX), "x")
    tokens_late, segments_late = lax.optimization_barrier((tokens, segments, column))[:2]
    pieces = ring(tokens_late, "tp")
    seg_before, seg_after = neighbours(segments_late)
    first_other = swap_core(first)
    seg_wide = jnp.concatenate([seg_before, segments_late, seg_after])
    seg_lanes = jnp.broadcast_to(seg_wide[:, None], (TOK + 2 * R, LANES))

    stream = tokens
    weights = (first, first_other)
    for layer in range(LAYERS):
        gated = gate(layer, at, pieces, in_gain, *weights)
        before, after = neighbours(gated)
        conv, stat = convolve(layer, before, gated, after, seg_lanes, jnp.swapaxes(conv_taps, 0, 1))
        stats = lax.all_gather(stat, "tp", axis=0, tiled=True)
        parts = project(layer, at, conv, stats, norm_gain, *weights)
        received = exchange(parts, "tp")
        stream = add_parts(stream, received)
        if layer == 0:
            rest = ring(after_(column[:, 3 * CH :], parts), "x")
            pieces = ring(stream, "tp")
            rest = jnp.stack(list(lax.optimization_barrier((*rest, stream))[:NX]))
            weights = (rest, swap_core(rest))
    return stream


def solution(mesh):
    fine = Mesh(mesh.devices.reshape(NZ, NX, NC, NT), ("z", "x", "c", "tp"))
    in_specs = (
        P(SP, "tp"),
        P(SP),
        P(),
        P(None, SP, "tp"),
        P(None, SP, "tp"),
        P(None, None, "tp"),
        P(None, "tp"),
        P(None, "tp", SP),
    )
    out_specs = P(SP, "tp")
    return jax.shard_map(program, mesh=fine, in_specs=in_specs, out_specs=out_specs, check_vma=False)
```

```python
import functools

import jax
import jax.numpy as jnp
from jax import lax
from jax.experimental import pallas as pl
from jax.experimental.pallas import tpu as pltpu
from jax.sharding import Mesh
from jax.sharding import PartitionSpec as P


D = 2048
CF = 1024
KW = 129
LAYERS = 2
EPSILON = 0.01
R = (KW - 1) // 2
SP = ("z", "x", "c")
NZ, NX, NC, NT = 16, 4, 2, 4
TOK = 256
CH = 256
FD = 512
LANES = 128
TILE = 64
STEPS = (0, 2, 1, 3)

F32 = jnp.float32
BF16 = jnp.bfloat16
LIMIT = pltpu.CompilerParams(vmem_limit_bytes=16 * 1024 * 1024)
VMEM = pl.BlockSpec(memory_space=pltpu.VMEM)
HBM = pl.BlockSpec(memory_space=pltpu.HBM)
SMEM = pl.BlockSpec(memory_space=pltpu.SMEM)


def assemble(at_ref, own_ref, other_ref, gate_ref, out_ref):
    core = at_ref[0]
    for i in range(NX):
        x = lax.rem(at_ref[2] + (NX - STEPS[i]), NX)
        for part, ref in ((core, own_ref), (1 - core, other_ref)):
            gate_ref[:, x, part] = ref[i, :, : 2 * CH].reshape(NZ, 16, 2 * CH)
            out_ref[:, x, part] = ref[i, :, 2 * CH :].reshape(NZ, 16, CH)


def pack_kernel(value_ref, gate_ref, out_ref, packed_ref, sems):
    copies = []
    for layer in range(LAYERS):
        for i, ref in enumerate((value_ref, gate_ref, out_ref)):
            n = 3 * layer + i
            target = packed_ref.at[:, n * CH : (n + 1) * CH]
            copies.append(pltpu.make_async_copy(ref.at[layer], target, sems.at[n]))
            copies[-1].start()
    for copy in copies:
        copy.wait()


def pack(value, gate_, out):
    return pl.pallas_call(
        pack_kernel,
        out_shape=jax.ShapeDtypeStruct((16, 6 * CH), BF16),
        in_specs=[HBM] * 3,
        out_specs=VMEM,
        scratch_shapes=[pltpu.SemaphoreType.DMA((6,))],
        name="pack",
    )(value, gate_, out)


def split_kernel(column_ref, first_ref, rest_ref):
    first_ref[...] = column_ref[:, : 3 * CH]
    rest_ref[...] = column_ref[:, 3 * CH :]


def split(column):
    return pl.pallas_call(
        split_kernel,
        out_shape=(jax.ShapeDtypeStruct((NZ * 16, 3 * CH), BF16),) * 2,
        in_specs=[VMEM],
        out_specs=(VMEM, VMEM),
        name="split",
        compiler_params=LIMIT,
    )(column)


def gate_kernel(layer, count, at_ref, *refs):
    *piece_refs, gain_ref, own_ref, other_ref, gated_ref, out_ref, w_ref = refs
    if count == 1:
        blocks = [(y, piece_refs[0][y]) for y in range(NT)]
    else:
        blocks = [(lax.rem(at_ref[1] + (NT - s), NT), ref[...]) for s, ref in zip(STEPS, piece_refs)]
    assemble(at_ref, own_ref, other_ref, w_ref, out_ref)
    wide = [block.astype(F32) for _, block in blocks]
    square = sum(jnp.sum(v * v, axis=1, keepdims=True) for v in wide)
    scale = lax.rsqrt(square * (1.0 / D) + EPSILON)
    pre = jnp.zeros((TOK, 2 * CH), F32)
    part = NZ // NT
    for v, (y, _) in zip(wide, blocks):
        start = y * FD if count == 1 else pl.multiple_of(y * FD, FD)
        gain = gain_ref[layer : layer + 1, pl.ds(start, FD)]
        normed = (v * scale * gain).astype(BF16)
        w = w_ref[pl.ds(y * part, part)].reshape(FD, 2 * CH)
        pre = pre + jnp.dot(normed, w, preferred_element_type=F32)
    gated_ref[...] = (pre[:, :CH] * jax.nn.sigmoid(pre[:, CH:])).astype(BF16)


def gate(layer, at, pieces, gain, own, other):
    return pl.pallas_call(
        functools.partial(gate_kernel, layer, len(pieces)),
        out_shape=(
            jax.ShapeDtypeStruct((TOK, CH), BF16),
            jax.ShapeDtypeStruct((NZ, NX, NC, 16, CH), BF16),
        ),
        in_specs=[SMEM] + [VMEM] * (3 + len(pieces)),
        out_specs=(VMEM, VMEM),
        scratch_shapes=[pltpu.VMEM((NZ, NX, NC, 16, 2 * CH), BF16)],
        name="gate",
        compiler_params=LIMIT,
    )(at, *pieces, gain, own, other)


def tap_sums(layer, x_ref, seg_ref, taps_ref, x_first, seg_first):
    own = seg_ref[seg_first + R : seg_first + R + TILE, :]
    acc = [jnp.zeros((TILE, LANES), F32) for _ in range(CH // LANES)]
    for k in range(KW):
        same = seg_ref[seg_first + k : seg_first + k + TILE, :] == own
        for h in range(CH // LANES):
            tap = taps_ref[k, layer : layer + 1, h * LANES : (h + 1) * LANES]
            window = x_ref[h, x_first + k : x_first + k + TILE, :]
            acc[h] = acc[h] + jnp.where(same, window * tap, 0.0)
    return acc


def inner_kernel(layer, mid_ref, seg_ref, taps_ref, conv_ref, x_ref):
    for h in range(CH // LANES):
        x_ref[h] = mid_ref[:, h * LANES : (h + 1) * LANES].astype(F32)
    for first in range(0, TOK - 2 * R, TILE):
        for h, acc in enumerate(tap_sums(layer, x_ref, seg_ref, taps_ref, first, first + R)):
            conv_ref[first : first + TILE, h * LANES : (h + 1) * LANES] = acc


def inner(layer, mid, seg, taps):
    return pl.pallas_call(
        functools.partial(inner_kernel, layer),
        out_shape=jax.ShapeDtypeStruct((TOK - 2 * R, CH), F32),
        in_specs=[VMEM] * 3,
        out_specs=VMEM,
        scratch_shapes=[pltpu.VMEM((CH // LANES, TOK, LANES), F32)],
        name="inner",
        compiler_params=LIMIT,
    )(mid, seg, taps)


def outer_kernel(layer, before_ref, mid_ref, after_ref, seg_ref, taps_ref, inner_ref, conv_ref, stat_ref, x_ref):
    for h in range(CH // LANES):
        cols = slice(h * LANES, (h + 1) * LANES)
        x_ref[h, 0:R] = before_ref[:, cols].astype(F32)
        x_ref[h, R : 3 * R] = mid_ref[: 2 * R, cols].astype(F32)
        x_ref[h, 3 * R : 5 * R] = mid_ref[TOK - 2 * R :, cols].astype(F32)
        x_ref[h, 5 * R :] = after_ref[:, cols].astype(F32)
    conv_ref[R : TOK - R, :] = inner_ref[...]
    for x_first, first in ((0, 0), (3 * R, TOK - R)):
        for h, acc in enumerate(tap_sums(layer, x_ref, seg_ref, taps_ref, x_first, first)):
            conv_ref[first : first + R, h * LANES : (h + 1) * LANES] = acc
    conv = conv_ref[...]
    ones = jnp.ones((8, CH), F32)
    dims = (((1,), (1,)), ((), ()))
    total = lax.dot_general(ones, conv, dims, precision=lax.Precision.HIGHEST, preferred_element_type=F32)
    square = lax.dot_general(ones, conv * conv, dims, precision=lax.Precision.HIGHEST, preferred_element_type=F32)
    for y in range(NT):
        stat_ref[y, 0:1, :] = total[0:1, :]
        stat_ref[y, 1:2, :] = square[0:1, :]


def outer(layer, before, mid, after, seg, taps, inside):
    return pl.pallas_call(
        functools.partial(outer_kernel, layer),
        out_shape=(jax.ShapeDtypeStruct((TOK, CH), F32), jax.ShapeDtypeStruct((NT, 2, TOK), F32)),
        in_specs=[VMEM] * 6,
        out_specs=(VMEM, VMEM),
        scratch_shapes=[pltpu.VMEM((CH // LANES, 6 * R, LANES), F32)],
        name="outer",
        compiler_params=LIMIT,
    )(before, mid, after, seg, taps, inside)


def out_kernel(layer, conv_ref, stat_ref, gain_ref, w_ref, parts_ref):
    stat = stat_ref[...]
    kind = lax.broadcasted_iota(jnp.int32, (2 * NT, CH), 0) % 2
    dims = (((0,), (0,)), ((), ()))

    def spread(which):
        pick = jnp.where(kind == which, 1.0, 0.0).astype(F32)
        return lax.dot_general(stat, pick, dims, precision=lax.Precision.HIGHEST, preferred_element_type=F32)

    mean = spread(0) * (1.0 / CF)
    var = jnp.maximum(spread(1) * (1.0 / CF) - mean * mean, 0.0)
    v = (conv_ref[...] - mean) * lax.rsqrt(var + EPSILON) * gain_ref[layer : layer + 1, :]
    act = jax.nn.silu(v).astype(BF16)
    rows = NZ // NT
    for y in range(NT):
        w = w_ref[y * rows : (y + 1) * rows].reshape(FD, CH)
        part = lax.dot_general(act, w, (((1,), (1,)), ((), ())), preferred_element_type=F32)
        parts_ref[y] = part.astype(BF16)


def project(layer, conv, stat, gain, weight):
    return pl.pallas_call(
        functools.partial(out_kernel, layer),
        out_shape=jax.ShapeDtypeStruct((NT, TOK, FD), BF16),
        in_specs=[VMEM] * 4,
        out_specs=VMEM,
        name="project",
        compiler_params=LIMIT,
    )(conv, stat, gain, weight)


def add_kernel(stream_ref, parts_ref, out_ref):
    total = stream_ref[...].astype(F32) + sum(parts_ref[y].astype(F32) for y in range(NT))
    out_ref[...] = total.astype(BF16)


def add_parts(stream, parts):
    return pl.pallas_call(
        add_kernel,
        out_shape=jax.ShapeDtypeStruct((TOK, FD), BF16),
        in_specs=[VMEM, VMEM],
        out_specs=VMEM,
        name="add_parts",
        compiler_params=LIMIT,
    )(stream, parts)


def copies_of(x, n):
    return jnp.broadcast_to(x[None], (n, *x.shape))


def swap_core(x):
    return lax.ppermute(x, "c", [(0, 1), (1, 0)])


def exchange(x, axis):
    return lax.all_to_all(x, axis, 0, 0, tiled=True)


def ring(pieces, axis):
    n = lax.axis_size(axis)
    came = [pieces[0]]
    for piece, step in zip(pieces[1:], STEPS[1:]):
        came.append(lax.ppermute(piece, axis, [(i, (i + step) % n) for i in range(n)]))
    return came


def neighbours(up, down):
    n = NZ * NX * NC
    ups = [(i, i + 1) for i in range(n - 1)]
    before = lax.ppermute(up, SP, ups)
    after = lax.ppermute(down, SP, [(j, i) for i, j in ups])
    return before, after


def after_(x, *others):
    return lax.optimization_barrier((x, *others))[0]


def program(tokens, segments, in_gain, w_value, w_gate, conv_taps, norm_gain, w_out):
    at = jnp.stack([lax.axis_index(a).astype(jnp.int32) for a in ("c", "tp", "x")])

    out_t = jnp.swapaxes(w_out, 1, 2)
    own = pack(w_value, w_gate, out_t)
    column = lax.all_gather(own, "z", axis=0, tiled=True)
    first_own, rest_own = split(column)
    first = ring([first_own] * NX, "x")
    tokens_late, segments_late = lax.optimization_barrier((tokens, segments, column))[:2]
    pieces = (exchange(copies_of(tokens_late, NT), "tp"),)
    seg_before, seg_after = neighbours(segments_late, segments_late)
    first = jnp.stack(first)
    first_other = swap_core(first)
    seg_wide = jnp.concatenate([seg_before[TOK - R :], segments, seg_after[:R]])
    seg_lanes = jnp.broadcast_to(seg_wide[:, None], (TOK + 2 * R, LANES))
    taps = jnp.swapaxes(conv_taps, 0, 1)

    stream = tokens
    weights = (first, first_other)
    for layer in range(LAYERS):
        gated, out_weight = gate(layer, at, pieces, in_gain, *weights)
        before, after = neighbours(gated[TOK - R :], gated[:R])
        inside = inner(layer, gated, seg_lanes, taps)
        conv, stat = outer(layer, before, gated, after, seg_lanes, taps, inside)
        stats = exchange(stat, "tp").reshape(2 * NT, TOK)
        parts = project(layer, conv, stats, norm_gain, out_weight)
        received = exchange(parts, "tp")
        stream = add_parts(stream, received)
        if layer == 0:
            rest = ring([after_(rest_own, parts)] * NX, "x")
            pieces = ring([stream] * NT, "tp")
            rest = jnp.stack(list(lax.optimization_barrier((*rest, stream))[:NX]))
            weights = (rest, swap_core(rest))
    return stream


def solution(mesh):
    fine = Mesh(mesh.devices.reshape(NZ, NX, NC, NT), ("z", "x", "c", "tp"))
    in_specs = (
        P(SP, "tp"),
        P(SP),
        P(),
        P(None, SP, "tp"),
        P(None, SP, "tp"),
        P(None, None, "tp"),
        P(None, "tp"),
        P(None, "tp", SP),
    )
    out_specs = P(SP, "tp")
    return jax.shard_map(
        program, mesh=fine, in_specs=in_specs, out_specs=out_specs, check_vma=False
    )
```

```python
import functools

import jax
import jax.numpy as jnp
from jax import lax
from jax.experimental import pallas as pl
from jax.experimental.pallas import tpu as pltpu
from jax.sharding import Mesh
from jax.sharding import PartitionSpec as P


D = 2048
CF = 1024
KW = 129
LAYERS = 2
EPSILON = 0.01
R = (KW - 1) // 2
SP = ("z", "x", "c")
NZ, NX, NC, NT = 16, 4, 2, 4
TOK = 256
CH = 256
FD = 512
LANES = 128
TILE = 64
STEPS = (0, 2, 1, 3)

F32 = jnp.float32
BF16 = jnp.bfloat16
LIMIT = pltpu.CompilerParams(vmem_limit_bytes=16 * 1024 * 1024)
VMEM = pl.BlockSpec(memory_space=pltpu.VMEM)
HBM = pl.BlockSpec(memory_space=pltpu.HBM)
SMEM = pl.BlockSpec(memory_space=pltpu.SMEM)


def assemble(rotated, at_ref, own_ref, other_ref, gate_ref, out_ref):
    core = at_ref[0]
    for i in range(NX):
        x = lax.rem(at_ref[2] + (NX - STEPS[i]), NX) if rotated else i
        for part, ref in ((core, own_ref), (1 - core, other_ref)):
            gate_ref[:, x, part] = ref[i, :, : 2 * CH].reshape(NZ, 16, 2 * CH)
            out_ref[:, x, part] = ref[i, :, 2 * CH :].reshape(NZ, 16, CH)


def pack_kernel(value_ref, gate_ref, out_ref, packed_ref, sems):
    copies = []
    for layer in range(LAYERS):
        for i, ref in enumerate((value_ref, gate_ref, out_ref)):
            n = 3 * layer + i
            target = packed_ref.at[:, n * CH : (n + 1) * CH]
            copies.append(pltpu.make_async_copy(ref.at[layer], target, sems.at[n]))
            copies[-1].start()
    for copy in copies:
        copy.wait()


def pack(value, gate_, out):
    return pl.pallas_call(
        pack_kernel,
        out_shape=jax.ShapeDtypeStruct((16, 6 * CH), BF16),
        in_specs=[HBM] * 3,
        out_specs=VMEM,
        scratch_shapes=[pltpu.SemaphoreType.DMA((6,))],
        name="pack",
    )(value, gate_, out)


def split_kernel(column_ref, first_ref, rest_ref):
    first_ref[...] = column_ref[:, : 3 * CH]
    rest_ref[...] = column_ref[:, 3 * CH :]


def split(column):
    return pl.pallas_call(
        split_kernel,
        out_shape=(jax.ShapeDtypeStruct((NZ * 16, 3 * CH), BF16),) * 2,
        in_specs=[VMEM],
        out_specs=(VMEM, VMEM),
        name="split",
        compiler_params=LIMIT,
    )(column)


def gate_kernel(layer, at_ref, *refs):
    *piece_refs, gain_ref, own_ref, other_ref, gated_ref, out_ref, w_ref = refs
    blocks = [(lax.rem(at_ref[1] + (NT - s), NT), ref[...]) for s, ref in zip(STEPS, piece_refs)]
    assemble(layer > 0, at_ref, own_ref, other_ref, w_ref, out_ref)
    wide = [block.astype(F32) for _, block in blocks]
    square = sum(jnp.sum(v * v, axis=1, keepdims=True) for v in wide)
    scale = lax.rsqrt(square * (1.0 / D) + EPSILON)
    pre = jnp.zeros((TOK, 2 * CH), F32)
    part = NZ // NT
    for v, (y, _) in zip(wide, blocks):
        start = pl.multiple_of(y * FD, FD)
        gain = gain_ref[layer : layer + 1, pl.ds(start, FD)]
        normed = (v * scale * gain).astype(BF16)
        w = w_ref[pl.ds(y * part, part)].reshape(FD, 2 * CH)
        pre = pre + jnp.dot(normed, w, preferred_element_type=F32)
    gated_ref[...] = (pre[:, :CH] * jax.nn.sigmoid(pre[:, CH:])).astype(BF16)


def gate(layer, at, pieces, gain, own, other):
    return pl.pallas_call(
        functools.partial(gate_kernel, layer),
        out_shape=(
            jax.ShapeDtypeStruct((TOK, CH), BF16),
            jax.ShapeDtypeStruct((NZ, NX, NC, 16, CH), BF16),
        ),
        in_specs=[SMEM] + [VMEM] * (3 + NT),
        out_specs=(VMEM, VMEM),
        scratch_shapes=[pltpu.VMEM((NZ, NX, NC, 16, 2 * CH), BF16)],
        name="gate",
        compiler_params=LIMIT,
    )(at, *pieces, gain, own, other)


def tap_sums(layer, x_ref, seg_ref, taps_ref, x_first, seg_first):
    own = seg_ref[seg_first + R : seg_first + R + TILE, :]
    acc = [jnp.zeros((TILE, LANES), F32) for _ in range(CH // LANES)]
    for k in range(KW):
        same = seg_ref[seg_first + k : seg_first + k + TILE, :] == own
        for h in range(CH // LANES):
            tap = taps_ref[k, layer : layer + 1, h * LANES : (h + 1) * LANES]
            window = x_ref[h, x_first + k : x_first + k + TILE, :]
            acc[h] = acc[h] + jnp.where(same, window * tap, 0.0)
    return acc


HALF = TOK - 2 * R


def inner_kernel(layer, own_ref, seg_ref, taps_ref, conv_ref, x_ref):
    for h in range(CH // LANES):
        x_ref[h] = own_ref[:, h * LANES : (h + 1) * LANES].astype(F32)
    for first in range(0, HALF, TILE):
        for h, acc in enumerate(tap_sums(layer, x_ref, seg_ref, taps_ref, first, first + (0, 2 * R)[layer])):
            conv_ref[first : first + TILE, h * LANES : (h + 1) * LANES] = acc


def inner(layer, own, seg, taps):
    return pl.pallas_call(
        functools.partial(inner_kernel, layer),
        out_shape=jax.ShapeDtypeStruct((HALF, CH), F32),
        in_specs=[VMEM] * 3,
        out_specs=VMEM,
        scratch_shapes=[pltpu.VMEM((CH // LANES, TOK, LANES), F32)],
        name="inner",
        compiler_params=LIMIT,
    )(own, seg, taps)


def lane_sums(wide):
    ones = jnp.ones((8, LANES), BF16)
    total = jnp.zeros((8, wide.shape[0]), F32)
    for _ in range(3):
        part = wide.astype(BF16)
        wide = wide - part.astype(F32)
        total = total + lax.dot_general(ones, part, (((1,), (1,)), ((), ())), preferred_element_type=F32)
    return total[0:1, :]


def outer_kernel(layer, own_ref, halo_ref, seg_ref, taps_ref, inner_ref, conv_ref, stat_ref, x_ref):
    for h in range(CH // LANES):
        cols = slice(h * LANES, (h + 1) * LANES)
        halo = halo_ref[:, cols].astype(F32)
        if layer == 0:
            x_ref[h, :HALF] = own_ref[TOK - HALF :, cols].astype(F32)
            x_ref[h, HALF:] = halo
        else:
            x_ref[h, : 2 * R] = halo
            x_ref[h, 2 * R :] = own_ref[:HALF, cols].astype(F32)
    skip, start = ((0, HALF), (2 * R, 0))[layer]
    conv_ref[skip : skip + HALF, :] = inner_ref[...]
    for first in range(0, 2 * R, TILE):
        for h, acc in enumerate(tap_sums(layer, x_ref, seg_ref, taps_ref, first, first + start)):
            conv_ref[start + first : start + first + TILE, h * LANES : (h + 1) * LANES] = acc
    low, high = conv_ref[:, :LANES], conv_ref[:, LANES:]
    for i, wide in enumerate((low + high, low * low + high * high)):
        row = lane_sums(wide)
        for y in range(NT):
            stat_ref[y, i : i + 1, :] = row


def outer(layer, own, halo, seg, taps, inside):
    return pl.pallas_call(
        functools.partial(outer_kernel, layer),
        out_shape=(jax.ShapeDtypeStruct((TOK, CH), F32), jax.ShapeDtypeStruct((NT, 2, TOK), F32)),
        in_specs=[VMEM] * 5,
        out_specs=(VMEM, VMEM),
        scratch_shapes=[pltpu.VMEM((CH // LANES, TOK, LANES), F32)],
        name="outer",
        compiler_params=LIMIT,
    )(own, halo, seg, taps, inside)


def out_kernel(layer, conv_ref, stat_ref, gain_ref, w_ref, parts_ref):
    stat = stat_ref[...]
    kind = lax.broadcasted_iota(jnp.int32, (2 * NT, LANES), 0) % 2
    dims = (((0,), (0,)), ((), ()))

    def spread(which):
        pick = jnp.where(kind == which, 1.0, 0.0).astype(F32)
        return lax.dot_general(stat, pick, dims, precision=lax.Precision.HIGHEST, preferred_element_type=F32)

    mean = spread(0) * (1.0 / CF)
    var = jnp.maximum(spread(1) * (1.0 / CF) - mean * mean, 0.0)
    scale = lax.rsqrt(var + EPSILON)
    act = []
    for h in range(CH // LANES):
        cols = slice(h * LANES, (h + 1) * LANES)
        v = (conv_ref[:, cols] - mean) * scale * gain_ref[layer : layer + 1, cols]
        act.append(jax.nn.silu(v).astype(BF16))
    act = jnp.concatenate(act, axis=1)
    rows = NZ // NT
    for y in range(NT):
        w = w_ref[y * rows : (y + 1) * rows].reshape(FD, CH)
        part = lax.dot_general(act, w, (((1,), (1,)), ((), ())), preferred_element_type=F32)
        parts_ref[y] = part.astype(BF16)


def project(layer, conv, stat, gain, weight):
    return pl.pallas_call(
        functools.partial(out_kernel, layer),
        out_shape=jax.ShapeDtypeStruct((NT, TOK, FD), BF16),
        in_specs=[VMEM] * 4,
        out_specs=VMEM,
        name="project",
        compiler_params=LIMIT,
    )(conv, stat, gain, weight)


def add_kernel(layer, stream_ref, side_ref, parts_ref, out_ref):
    def part(rows):
        return sum(parts_ref[y, rows].astype(F32) for y in range(NT))

    if layer == 0:
        kept, own, side = slice(R, TOK), slice(0, TOK - R), slice(TOK - R, TOK)
    else:
        kept, own, side = slice(0, TOK - R), slice(R, TOK), slice(0, R)
    out_ref[own] = (stream_ref[kept].astype(F32) + part(own)).astype(BF16)
    out_ref[side] = (side_ref[...].astype(F32) + part(side)).astype(BF16)


def add_parts(layer, stream, side, parts):
    return pl.pallas_call(
        functools.partial(add_kernel, layer),
        out_shape=jax.ShapeDtypeStruct((TOK, FD), BF16),
        in_specs=[VMEM] * 3,
        out_specs=VMEM,
        name="add_parts",
        compiler_params=LIMIT,
    )(stream, side, parts)


def copies_of(x, n):
    return jnp.broadcast_to(x[None], (n, *x.shape))


def swap_core(x):
    return lax.ppermute(x, "c", [(0, 1), (1, 0)])


def exchange(x, axis):
    return lax.all_to_all(x, axis, 0, 0, tiled=True)


def ring(pieces, axis):
    n = lax.axis_size(axis)
    came = [pieces[0]]
    for piece, step in zip(pieces[1:], STEPS[1:]):
        came.append(lax.ppermute(piece, axis, [(i, (i + step) % n) for i in range(n)]))
    return came


def from_next(x):
    n = NZ * NX * NC
    return lax.ppermute(x, SP, [((i + 1) % n, i) for i in range(n)])


def from_previous(x):
    n = NZ * NX * NC
    return lax.ppermute(x, SP, [(i, (i + 1) % n) for i in range(n)])


def after_(x, *others):
    return lax.optimization_barrier((x, *others))[0]


def program(tokens, segments, in_gain, w_value, w_gate, conv_taps, norm_gain, w_out):
    at = jnp.stack([lax.axis_index(a).astype(jnp.int32) for a in ("c", "tp", "x")])

    out_t = jnp.swapaxes(w_out, 1, 2)
    own = pack(w_value, w_gate, out_t)
    column = lax.all_gather(own, "z", axis=0, tiled=True)
    first_own, rest_own = split(column)
    first = exchange(copies_of(first_own, NX), "x")
    tokens_late, segments_late = lax.optimization_barrier((tokens, segments, column))[:2]
    pieces = ring([tokens_late] * NT, "tp")
    seg_after = from_next(segments_late)
    first_other = swap_core(first)

    def seg_rows(*pieces):
        return jnp.broadcast_to(jnp.concatenate(pieces)[:, None], (TOK + 2 * R, LANES))

    seg_lanes = seg_rows(segments, seg_after[: 2 * R])
    taps = jnp.swapaxes(conv_taps, 0, 1)

    stream = tokens
    weights = (first, first_other)
    for layer in range(LAYERS):
        gated, out_weight = gate(layer, at, pieces, in_gain, *weights)
        if layer == 0:
            halo = from_next(gated[: 2 * R])
        else:
            halo = from_previous(gated[TOK - 2 * R :])
        inside = inner(layer, gated, seg_lanes, taps)
        conv, stat = outer(layer, gated, halo, seg_lanes, taps, inside)
        stats = exchange(stat, "tp").reshape(2 * NT, TOK)
        if layer == 0:
            tokens_after = from_next(after_(tokens, conv)[:R])
        parts = project(layer, conv, stats, norm_gain, out_weight)
        received = exchange(parts, "tp")
        side = tokens_after if layer == 0 else stream_before
        stream = add_parts(layer, stream, side, received)
        if layer == 0:
            stream_before = from_previous(stream[TOK - R :])
            seg_before = from_previous(after_(segments, stream))
            seg_lanes = seg_rows(seg_before[TOK - R :], segments, seg_after[:R])
            rest = ring([after_(rest_own, parts)] * NX, "x")
            pieces = ring([stream] * NT, "tp")
            rest = jnp.stack(list(lax.optimization_barrier((*rest, stream))[:NX]))
            weights = (rest, swap_core(rest))
    return stream


def solution(mesh):
    fine = Mesh(mesh.devices.reshape(NZ, NX, NC, NT), ("z", "x", "c", "tp"))
    in_specs = (
        P(SP, "tp"),
        P(SP),
        P(),
        P(None, SP, "tp"),
        P(None, SP, "tp"),
        P(None, None, "tp"),
        P(None, "tp"),
        P(None, "tp", SP),
    )
    out_specs = P(SP, "tp")
    return jax.shard_map(
        program, mesh=fine, in_specs=in_specs, out_specs=out_specs, check_vma=False
    )
```

```python
import functools

import jax
import jax.numpy as jnp
from jax import lax
from jax.experimental import pallas as pl
from jax.experimental.pallas import tpu as pltpu
from jax.sharding import Mesh
from jax.sharding import PartitionSpec as P


D = 2048
CF = 1024
KW = 129
LAYERS = 2
EPSILON = 0.01
R = (KW - 1) // 2
SP = ("z", "x", "c")
NZ, NX, NC, NT = 16, 4, 2, 4
TOK = 256
CH = 256
FD = 512
LANES = 128
TILE = 64
STEPS = (0, 2, 1, 3)

F32 = jnp.float32
BF16 = jnp.bfloat16
LIMIT = pltpu.CompilerParams(vmem_limit_bytes=16 * 1024 * 1024)
VMEM = pl.BlockSpec(memory_space=pltpu.VMEM)
HBM = pl.BlockSpec(memory_space=pltpu.HBM)
SMEM = pl.BlockSpec(memory_space=pltpu.SMEM)


def assemble(rotated, at_ref, own_ref, other_ref, gate_ref, out_ref):
    core = at_ref[0]
    for i in range(NX):
        x = lax.rem(at_ref[2] + (NX - STEPS[i]), NX) if rotated else i
        for part, ref in ((core, own_ref), (1 - core, other_ref)):
            gate_ref[:, x, part] = ref[i, :, : 2 * CH].reshape(NZ, 16, 2 * CH)
            out_ref[:, x, part] = ref[i, :, 2 * CH :].reshape(NZ, 16, CH)


def pack_kernel(value_ref, gate_ref, out_ref, packed_ref, sems):
    copies = []
    for layer in range(LAYERS):
        for i, ref in enumerate((value_ref, gate_ref, out_ref)):
            n = 3 * layer + i
            target = packed_ref.at[:, n * CH : (n + 1) * CH]
            copies.append(pltpu.make_async_copy(ref.at[layer], target, sems.at[n]))
            copies[-1].start()
    for copy in copies:
        copy.wait()


def pack(value, gate_, out):
    return pl.pallas_call(
        pack_kernel,
        out_shape=jax.ShapeDtypeStruct((16, 6 * CH), BF16),
        in_specs=[HBM] * 3,
        out_specs=VMEM,
        scratch_shapes=[pltpu.SemaphoreType.DMA((6,))],
        name="pack",
    )(value, gate_, out)


def split_kernel(column_ref, first_ref, rest_ref):
    for x in range(NX):
        first_ref[x] = column_ref[:, : 3 * CH]
    rest_ref[...] = column_ref[:, 3 * CH :]


def split(column):
    return pl.pallas_call(
        split_kernel,
        out_shape=(
            jax.ShapeDtypeStruct((NX, NZ * 16, 3 * CH), BF16),
            jax.ShapeDtypeStruct((NZ * 16, 3 * CH), BF16),
        ),
        in_specs=[VMEM],
        out_specs=(VMEM, VMEM),
        name="split",
        compiler_params=LIMIT,
    )(column)


def gate_kernel(layer, at_ref, *refs):
    *piece_refs, gain_ref, own_ref, other_ref, gated_ref, out_ref, w_ref = refs
    blocks = [(lax.rem(at_ref[1] + (NT - s), NT), ref[...]) for s, ref in zip(STEPS, piece_refs)]
    assemble(layer > 0, at_ref, own_ref, other_ref, w_ref, out_ref)
    wide = [block.astype(F32) for _, block in blocks]
    square = sum(jnp.sum(v * v, axis=1, keepdims=True) for v in wide)
    scale = lax.rsqrt(square * (1.0 / D) + EPSILON)
    pre = jnp.zeros((TOK, 2 * CH), F32)
    part = NZ // NT
    for v, (y, _) in zip(wide, blocks):
        start = pl.multiple_of(y * FD, FD)
        gain = gain_ref[layer : layer + 1, pl.ds(start, FD)]
        normed = (v * scale * gain).astype(BF16)
        w = w_ref[pl.ds(y * part, part)].reshape(FD, 2 * CH)
        pre = pre + jnp.dot(normed, w, preferred_element_type=F32)
    gated_ref[...] = (pre[:, :CH] * jax.nn.sigmoid(pre[:, CH:])).astype(BF16)


def gate(layer, at, pieces, gain, own, other):
    return pl.pallas_call(
        functools.partial(gate_kernel, layer),
        out_shape=(
            jax.ShapeDtypeStruct((TOK, CH), BF16),
            jax.ShapeDtypeStruct((NZ, NX, NC, 16, CH), BF16),
        ),
        in_specs=[SMEM] + [VMEM] * (3 + NT),
        out_specs=(VMEM, VMEM),
        scratch_shapes=[pltpu.VMEM((NZ, NX, NC, 16, 2 * CH), BF16)],
        name="gate",
        compiler_params=LIMIT,
    )(at, *pieces, gain, own, other)


def tap_sums(layer, x_ref, seg_ref, taps_ref, x_first, seg_first):
    own = seg_ref[seg_first + R : seg_first + R + TILE, :]
    acc = [jnp.zeros((TILE, LANES), F32) for _ in range(CH // LANES)]
    for k in range(KW):
        same = seg_ref[seg_first + k : seg_first + k + TILE, :] == own
        for h in range(CH // LANES):
            tap = taps_ref[k, layer : layer + 1, h * LANES : (h + 1) * LANES]
            window = x_ref[h, x_first + k : x_first + k + TILE, :]
            acc[h] = acc[h] + jnp.where(same, window * tap, 0.0)
    return acc


HALF = TOK - 2 * R


def inner_kernel(layer, own_ref, seg_ref, taps_ref, conv_ref, x_ref):
    for h in range(CH // LANES):
        x_ref[h] = own_ref[:, h * LANES : (h + 1) * LANES].astype(F32)
    for first in range(0, HALF, TILE):
        for h, acc in enumerate(tap_sums(layer, x_ref, seg_ref, taps_ref, first, first + (0, 2 * R)[layer])):
            conv_ref[first : first + TILE, h * LANES : (h + 1) * LANES] = acc


def inner(layer, own, seg, taps):
    return pl.pallas_call(
        functools.partial(inner_kernel, layer),
        out_shape=jax.ShapeDtypeStruct((HALF, CH), F32),
        in_specs=[VMEM] * 3,
        out_specs=VMEM,
        scratch_shapes=[pltpu.VMEM((CH // LANES, TOK, LANES), F32)],
        name="inner",
        compiler_params=LIMIT,
    )(own, seg, taps)


def lane_sums(wide):
    ones = jnp.ones((8, LANES), BF16)
    total = jnp.zeros((8, wide.shape[0]), F32)
    for _ in range(3):
        part = wide.astype(BF16)
        wide = wide - part.astype(F32)
        total = total + lax.dot_general(ones, part, (((1,), (1,)), ((), ())), preferred_element_type=F32)
    return total[0:1, :]


def outer_kernel(layer, own_ref, halo_ref, seg_ref, taps_ref, inner_ref, conv_ref, stat_ref, x_ref):
    for h in range(CH // LANES):
        cols = slice(h * LANES, (h + 1) * LANES)
        halo = halo_ref[:, cols].astype(F32)
        if layer == 0:
            x_ref[h, :HALF] = own_ref[TOK - HALF :, cols].astype(F32)
            x_ref[h, HALF:] = halo
        else:
            x_ref[h, : 2 * R] = halo
            x_ref[h, 2 * R :] = own_ref[:HALF, cols].astype(F32)
    skip, start = ((0, HALF), (2 * R, 0))[layer]
    conv_ref[skip : skip + HALF, :] = inner_ref[...]
    for first in range(0, 2 * R, TILE):
        for h, acc in enumerate(tap_sums(layer, x_ref, seg_ref, taps_ref, first, first + start)):
            conv_ref[start + first : start + first + TILE, h * LANES : (h + 1) * LANES] = acc
    low, high = conv_ref[:, :LANES], conv_ref[:, LANES:]
    for i, wide in enumerate((low + high, low * low + high * high)):
        row = lane_sums(wide)
        for y in range(NT):
            stat_ref[y, i : i + 1, :] = row


def outer(layer, own, halo, seg, taps, inside):
    return pl.pallas_call(
        functools.partial(outer_kernel, layer),
        out_shape=(jax.ShapeDtypeStruct((TOK, CH), F32), jax.ShapeDtypeStruct((NT, 2, TOK), F32)),
        in_specs=[VMEM] * 5,
        out_specs=(VMEM, VMEM),
        scratch_shapes=[pltpu.VMEM((CH // LANES, TOK, LANES), F32)],
        name="outer",
        compiler_params=LIMIT,
    )(own, halo, seg, taps, inside)


def out_kernel(layer, conv_ref, stat_ref, gain_ref, w_ref, parts_ref):
    stat = stat_ref[...]
    kind = lax.broadcasted_iota(jnp.int32, (2 * NT, LANES), 0) % 2
    dims = (((0,), (0,)), ((), ()))

    def spread(which):
        pick = jnp.where(kind == which, 1.0, 0.0).astype(F32)
        return lax.dot_general(stat, pick, dims, precision=lax.Precision.HIGHEST, preferred_element_type=F32)

    mean = spread(0) * (1.0 / CF)
    var = jnp.maximum(spread(1) * (1.0 / CF) - mean * mean, 0.0)
    scale = lax.rsqrt(var + EPSILON)
    act = []
    for h in range(CH // LANES):
        cols = slice(h * LANES, (h + 1) * LANES)
        v = (conv_ref[:, cols] - mean) * scale * gain_ref[layer : layer + 1, cols]
        act.append(jax.nn.silu(v).astype(BF16))
    act = jnp.concatenate(act, axis=1)
    rows = NZ // NT
    for y in range(NT):
        w = w_ref[y * rows : (y + 1) * rows].reshape(FD, CH)
        part = lax.dot_general(act, w, (((1,), (1,)), ((), ())), preferred_element_type=F32)
        parts_ref[y] = part.astype(BF16)


def project(layer, conv, stat, gain, weight):
    return pl.pallas_call(
        functools.partial(out_kernel, layer),
        out_shape=jax.ShapeDtypeStruct((NT, TOK, FD), BF16),
        in_specs=[VMEM] * 4,
        out_specs=VMEM,
        name="project",
        compiler_params=LIMIT,
    )(conv, stat, gain, weight)


def add_kernel(layer, stream_ref, side_ref, parts_ref, out_ref):
    def part(rows):
        return sum(parts_ref[y, rows].astype(F32) for y in range(NT))

    if layer == 0:
        kept, own, side = slice(R, TOK), slice(0, TOK - R), slice(TOK - R, TOK)
    else:
        kept, own, side = slice(0, TOK - R), slice(R, TOK), slice(0, R)
    out_ref[own] = (stream_ref[kept].astype(F32) + part(own)).astype(BF16)
    out_ref[side] = (side_ref[...].astype(F32) + part(side)).astype(BF16)


def add_parts(layer, stream, side, parts):
    return pl.pallas_call(
        functools.partial(add_kernel, layer),
        out_shape=jax.ShapeDtypeStruct((TOK, FD), BF16),
        in_specs=[VMEM] * 3,
        out_specs=VMEM,
        name="add_parts",
        compiler_params=LIMIT,
    )(stream, side, parts)


def swap_core(x):
    return lax.ppermute(x, "c", [(0, 1), (1, 0)])


def exchange(x, axis):
    return lax.all_to_all(x, axis, 0, 0, tiled=True)


def ring(pieces, axis):
    n = lax.axis_size(axis)
    came = [pieces[0]]
    for piece, step in zip(pieces[1:], STEPS[1:]):
        came.append(lax.ppermute(piece, axis, [(i, (i + step) % n) for i in range(n)]))
    return came


def from_next(x):
    n = NZ * NX * NC
    return lax.ppermute(x, SP, [((i + 1) % n, i) for i in range(n)])


def from_previous(x):
    n = NZ * NX * NC
    return lax.ppermute(x, SP, [(i, (i + 1) % n) for i in range(n)])


def after_(x, *others):
    return lax.optimization_barrier((x, *others))[0]


def program(tokens, segments, in_gain, w_value, w_gate, conv_taps, norm_gain, w_out):
    at = jnp.stack([lax.axis_index(a).astype(jnp.int32) for a in ("c", "tp", "x")])

    out_t = jnp.swapaxes(w_out, 1, 2)
    own = pack(w_value, w_gate, out_t)
    column = lax.all_gather(own, "z", axis=0, tiled=True)
    first_copies, rest_own = split(column)
    first = exchange(first_copies, "x")
    tokens_late, segments_late = lax.optimization_barrier((tokens, segments, column))[:2]
    pieces = ring([tokens_late] * NT, "tp")
    tokens_head = tokens_late[:R]
    seg_after = from_next(segments_late)
    seg_before = from_previous(segments_late)
    first_other = swap_core(first)

    def seg_rows(*pieces):
        return jnp.broadcast_to(jnp.concatenate(pieces)[:, None], (TOK + 2 * R, LANES))

    seg_lanes = seg_rows(segments, seg_after[: 2 * R])
    taps = jnp.swapaxes(conv_taps, 0, 1)

    stream = tokens
    weights = (first, first_other)
    for layer in range(LAYERS):
        gated, out_weight = gate(layer, at, pieces, in_gain, *weights)
        if layer == 0:
            halo = from_next(gated[: 2 * R])
        else:
            halo = from_previous(gated[TOK - 2 * R :])
        inside = inner(layer, gated, seg_lanes, taps)
        conv, stat = outer(layer, gated, halo, seg_lanes, taps, inside)
        stats = exchange(stat, "tp").reshape(2 * NT, TOK)
        if layer == 0:
            tokens_after = from_next(after_(tokens_head, conv))
        parts = project(layer, conv, stats, norm_gain, out_weight)
        received = exchange(parts, "tp")
        side = tokens_after if layer == 0 else stream_before
        stream = add_parts(layer, stream, side, received)
        if layer == 0:
            stream_before = from_previous(stream[TOK - R :])
            seg_lanes = seg_rows(after_(seg_before, stream)[TOK - R :], segments, seg_after[:R])
            rest = ring([after_(rest_own, parts)] * NX, "x")
            pieces = ring([stream] * NT, "tp")
            rest = jnp.stack(list(lax.optimization_barrier((*rest, stream))[:NX]))
            weights = (rest, swap_core(rest))
    return stream


def solution(mesh):
    fine = Mesh(mesh.devices.reshape(NZ, NX, NC, NT), ("z", "x", "c", "tp"))
    in_specs = (
        P(SP, "tp"),
        P(SP),
        P(),
        P(None, SP, "tp"),
        P(None, SP, "tp"),
        P(None, None, "tp"),
        P(None, "tp"),
        P(None, "tp", SP),
    )
    out_specs = P(SP, "tp")
    return jax.shard_map(
        program, mesh=fine, in_specs=in_specs, out_specs=out_specs, check_vma=False
    )
```
